32 devices in a mesh: ep: 8 (over z, y), tp: 4 (over x, core).
Axes of the slice: x: 2, y: 2, z: 4, core: 2. Of those that a mesh axis runs over, the one named last changes fastest.
Arguments:
- queries: bfloat16 [4096, 1024], P('ep', 'tp'), may hold values from -10.5 to 10.5
- keys: bfloat16 [4096, 512], P('ep', 'tp'), may hold values from -10.5 to 10.5
- values: bfloat16 [4096, 512], P('ep', 'tp'), may hold values from -6 to 6
- head_lambda: float32 [8], P('tp'), may hold values from 0.3 to 0.8
- out_gain: float32 [128], replicated, may hold values from 0.1 to 1.9
- expert_input: bfloat16 [4096, 2048], P(('ep', 'tp')), may hold values from -6 to 6
- routes: int32 [4096, 4], P(('ep', 'tp')), may hold values from 0 to 7, all different within a row; in each aligned block of 128 rows (0 to 127, 128 to 255, ...) at most 80 rows name the same one
- route_weight: float32 [4096, 4], P(('ep', 'tp')), may hold values from 0.2 to 0.6
- moe_gain: float32 [2048], replicated, may hold values from 0.1 to 1.9
- gate_weight: bfloat16 [8, 2048, 2048], P('ep', None, 'tp'), may hold values from -0.3125 to 0.3125
- up_weight: bfloat16 [8, 2048, 2048], P('ep', None, 'tp'), may hold values from -0.3125 to 0.3125
- down_weight: bfloat16 [8, 2048, 2048], P('ep', 'tp'), may hold values from -0.03125 to 0.03125
Outputs:
- mixed_out: bfloat16 [4096, 1024], P('ep', 'tp')
- expert_mix: bfloat16 [4096, 2048], P(('ep', 'tp'))
The draws below stay inside these ranges and needn't reach their ends.
Inputs may be any that keep to these rules, and one draw needn't show every extreme that they name: `routes`: each row names 4 different experts. Among the rows of one device (aligned blocks of 128 rows) no expert is named more than 80 times, and in some blocks one is named exactly 80 times.
All inputs are finite; a program needn't handle non-finite values.
Results may differ from the reference program's by a relative error of at most 0.012.
Values may be sent and summed in bfloat16 or wider, within the bound.
A program may use at most 128 MiB of HBM per device.

```python
import math
import jax
import jax.numpy as jnp
import numpy as np
from jax import lax

D = 2048
HEADS = 8
KV_HEADS = 4
HEAD = 64
VDIM = 128
FF = 2048
TOPK = 4
TOK_DEV = 128
LEN = 4096
TOKENS = 4096
EXPERTS = 8
CAP = 80
N_EP = 8
N_TP = 4


def draw_queries(key, part):
    folded = jax.random.fold_in(key, 101)
    drawn_field = jnp.clip(jax.random.normal(folded, (LEN, HEADS, 2, HEAD), jnp.float32) * 1.32, -7.9, 7.9)
    return drawn_field.reshape(LEN, HEADS * 2 * HEAD).astype(jnp.bfloat16)


def draw_keys(key, part):
    folded = jax.random.fold_in(key, 202)
    drawn_field = jnp.clip(jax.random.normal(folded, (LEN, KV_HEADS, 2, HEAD), jnp.float32) * 1.32, -7.9, 7.9)
    return drawn_field.reshape(LEN, KV_HEADS * 2 * HEAD).astype(jnp.bfloat16)


def block_scale(stream_key, extent, cuts, least, largest):
    gain = 1.0
    for axis_at, shards_of in cuts:
        draws = jax.random.uniform(jax.random.fold_in(jax.random.fold_in(stream_key, 6), axis_at), (shards_of,), jnp.float32, least / len(cuts), largest / len(cuts))
        gain = gain * jnp.repeat(jnp.exp(draws), extent[axis_at] // shards_of).reshape((-1,) + (1,) * (len(extent) - 1 - axis_at))
    return gain


def assign_block(stream_key, own, number, rows, count, top, most, skew):
    order = jax.random.permutation(stream_key, count)
    crowded, ordinary = load_shares(count, rows * top, most, skew, True), load_shares(count, rows * top, most, skew, False)
    places = jnp.arange(count)

    def named(tallies, rotation):
        used = int((tallies > 0).sum())
        fixed = max(1, used // 4)
        moved = fixed + (places - fixed + rotation * (used - fixed)) % max(1, count - fixed)
        return jnp.zeros((count,), jnp.int32).at[order[jnp.where(places < fixed, places, moved)]].set(jnp.asarray(tallies, jnp.int32))

    tallies = jnp.where(number % 4 == 0, named(crowded, number // 4), named(ordinary, number - number // 4 - 1))
    mixed = jax.random.permutation(jax.random.fold_in(own, 3), count)
    donor, receiver = mixed[0:count // 2 * 2:2], mixed[1:count // 2 * 2:2]
    margin = jnp.minimum(tallies[donor] - 1, most - tallies[receiver]) // 2
    margin = jnp.where((donor == order[0]) | (receiver == order[0]) | (tallies[receiver] == 0), 0, jnp.maximum(margin, 0))
    moved = jax.random.randint(jax.random.fold_in(own, 4), (count // 2,), 0, 1 << 20) % (margin + 1)
    tallies = tallies.at[donor].add(-moved).at[receiver].add(moved)
    items = jnp.searchsorted(jnp.cumsum(tallies), jnp.arange(rows * top), side="right").astype(jnp.int32)
    listing = items.reshape(top, rows).T
    listing = listing[jax.random.permutation(jax.random.fold_in(own, 1), rows)]
    rotation = jax.random.randint(jax.random.fold_in(own, 2), (rows, 1), 0, top)
    return jnp.take_along_axis(listing, (jnp.arange(top)[None, :] + rotation) % top, axis=1)


def load_shares(amount, total, most, lean, full):
    loads = [(1 << 20) // math.isqrt(standing ** lean) + 1 for standing in range(1, amount + 1)]
    largest = most if full else min(most, max(-(-total // amount), total * loads[0] // sum(loads)))
    least = 1 if total - largest >= amount - 1 else 0
    given, rest = [largest] + [least] * (amount - 1), total - largest - least * (amount - 1)
    while rest > 0:
        movable = [i for i in range(1, amount) if given[i] < largest] or [i for i in range(1, amount) if given[i] < most]
        whole, budget = sum([loads[i] for i in movable]), rest
        for i in movable:
            addition = min(most - given[i], max(1, budget * loads[i] // whole), rest)
            given[i] = given[i] + addition
            rest = rest - addition
    return np.array(given)


def gaussian(rng, extent, deviation, reach, cuts=(), kind=jnp.bfloat16):
    values = jax.random.normal(rng, extent, jnp.float32) * deviation
    if len(cuts) > 0:
        values = block_scale(rng, extent, cuts, -0.22, 0.18) * values
    return jnp.clip(values, min=-reach, max=reach).astype(kind)


def setup_inputs(seed: int = 0) -> dict:
    arg_keys = jax.random.split(jax.random.key(seed), 13)
    queries = draw_queries(jax.random.fold_in(arg_keys[12], 71), 0)
    keys = draw_keys(jax.random.fold_in(arg_keys[12], 71), 0)
    values = gaussian(arg_keys[2], (LEN, KV_HEADS * VDIM), 1.0, 6.0, ((0, 8), (1, 4)))
    head_lambda = jnp.clip(0.3 + 0.5 * jax.random.uniform(arg_keys[3], (HEADS,), jnp.float32) ** block_scale(arg_keys[3], (HEADS,), ((0, 4),), -0.2, 0.2), 0.3, 0.8)
    out_gain = jnp.clip(1.0 + 0.18 * jax.random.normal(arg_keys[4], (VDIM,), jnp.float32), 0.1, 1.9)
    expert_input = gaussian(arg_keys[5], (TOKENS, D), 1.0, 6.0, ((0, 32),))
    routes_keys = jax.random.split(jax.random.fold_in(arg_keys[6], 1), TOKENS // TOK_DEV)
    routes_turns = jax.random.permutation(jax.random.fold_in(arg_keys[6], 3), TOKENS // TOK_DEV)
    routes = jax.vmap(lambda own, number: assign_block(jax.random.fold_in(arg_keys[6], 2), own, number, TOK_DEV, EXPERTS, TOPK, CAP, 2))(routes_keys, routes_turns).reshape((TOKENS, TOPK))
    route_weight = jnp.clip(0.2 + 0.400000021 * jax.random.uniform(arg_keys[7], (TOKENS, TOPK), jnp.float32) ** block_scale(arg_keys[7], (TOKENS, TOPK), ((0, 32),), -0.2, 0.2), 0.2, 0.6)
    moe_gain = jnp.clip(1.0 + 0.18 * jax.random.normal(arg_keys[8], (D,), jnp.float32), 0.1, 1.9)
    gate_weight = gaussian(arg_keys[9], (EXPERTS, D, FF), (D // 6) ** -0.5, 0.3125, ((0, 8), (2, 4)))
    up_weight = gaussian(arg_keys[10], (EXPERTS, D, FF), (D // 6) ** -0.5, 0.3125, ((0, 8), (2, 4)))
    down_weight = gaussian(arg_keys[11], (EXPERTS, FF, D), (FF * 16) ** -0.5, 0.03125, ((0, 8), (1, 4)))
    return dict(queries=queries, keys=keys, values=values, head_lambda=head_lambda, out_gain=out_gain, expert_input=expert_input, routes=routes, route_weight=route_weight, moe_gain=moe_gain, gate_weight=gate_weight, up_weight=up_weight, down_weight=down_weight)


epsilon = 1e-05

def attention(queries, keys, values, head_lambda, out_gain):
    group_size = HEADS // KV_HEADS
    block_len = math.gcd(LEN, 512)
    score_scale = HEAD ** (-0.5)
    positions = jnp.arange(LEN, dtype=jnp.int32)

    def one_head(head_index):
        kv_index = head_index // group_size
        head_queries = lax.dynamic_slice_in_dim(queries, head_index * (2 * HEAD), 2 * HEAD, 1).reshape(LEN, 2, HEAD).astype(jnp.float32)
        head_keys = lax.dynamic_slice_in_dim(keys, kv_index * (2 * HEAD), 2 * HEAD, 1).reshape(LEN, 2, HEAD).astype(jnp.float32)
        head_values = lax.dynamic_slice_in_dim(values, kv_index * VDIM, VDIM, 1).astype(jnp.float32)
        weight_lambda = head_lambda[head_index]

        def one_block(block_index):
            query_block = lax.dynamic_slice_in_dim(head_queries, block_index * block_len, block_len, 0)
            scores = jnp.einsum('tmd,smd->mts', query_block, head_keys) * score_scale
            query_pos = block_index * block_len + jnp.arange(block_len, dtype=jnp.int32)
            allowed = (positions[None, :] <= query_pos[:, None])[None]
            masked = jnp.where(allowed, scores, -jnp.inf)
            row_max = lax.optimization_barrier(jnp.max(masked, axis=-1, keepdims=True))
            weights = jnp.where(allowed, jnp.exp(scores - row_max), 0.0)
            totals = lax.optimization_barrier(jnp.sum(weights, axis=-1))
            rounded = lax.optimization_barrier(weights.astype(jnp.bfloat16))
            summed = jnp.einsum('mts,sv->mtv', rounded.astype(jnp.float32), head_values)
            return summed[0] / totals[0][:, None] - weight_lambda * summed[1] / totals[1][:, None]
        return lax.map(one_block, jnp.arange(LEN // block_len, dtype=jnp.int32)).reshape(LEN, VDIM)
    combined = lax.map(one_head, jnp.arange(HEADS, dtype=jnp.int32))
    inverse_rms = lax.rsqrt(lax.optimization_barrier(jnp.mean(combined * combined, axis=-1, keepdims=True)) + epsilon)
    mixed_out = (combined * inverse_rms * out_gain).astype(jnp.bfloat16)
    return jnp.transpose(mixed_out, (1, 0, 2)).reshape(LEN, HEADS * VDIM)

def experts_part(expert_input, routes, route_weight, moe_gain, gate_weight, up_weight, down_weight):
    most_rows = N_EP * N_TP * CAP
    hidden_block = FF // N_TP
    inputs_f32 = expert_input.astype(jnp.float32)
    normed = (inputs_f32 * lax.rsqrt(lax.optimization_barrier(jnp.mean(inputs_f32 * inputs_f32, axis=-1, keepdims=True)) + epsilon) * moe_gain).astype(jnp.bfloat16)
    flat_routes = routes.reshape(-1)
    flat_weights = route_weight.reshape(-1)

    def one_expert(totals, expert_index):
        matches = flat_routes == expert_index
        chosen = jnp.nonzero(matches, size=most_rows, fill_value=0)[0].astype(jnp.int32)
        live_rows = (jnp.arange(most_rows, dtype=jnp.int32) < jnp.sum(matches.astype(jnp.int32))).astype(jnp.float32)
        token_rows = chosen // TOPK
        rows_in = normed[token_rows]
        gate_pre = jnp.dot(rows_in, gate_weight[expert_index], preferred_element_type=jnp.float32)
        up_pre = jnp.dot(rows_in, up_weight[expert_index], preferred_element_type=jnp.float32)
        clipped = jnp.minimum(gate_pre, 7.0)
        up_clip = jnp.clip(up_pre, -7.0, 7.0)
        activation = ((up_clip + 1.0) * clipped * jax.nn.sigmoid(1.702 * clipped)).astype(jnp.bfloat16)
        partial_value = jnp.einsum('rnf,nfd->nrd', activation.reshape(most_rows, N_TP, hidden_block).astype(jnp.float32), down_weight[expert_index].reshape(N_TP, hidden_block, D).astype(jnp.float32))
        rounded = lax.optimization_barrier(partial_value.astype(jnp.bfloat16)).astype(jnp.float32)
        expert_out = lax.optimization_barrier(jnp.sum(rounded, axis=0)).astype(jnp.bfloat16)
        contribution = expert_out.astype(jnp.float32) * (flat_weights[chosen] * live_rows)[:, None]
        return (totals.at[token_rows].add(contribution), None)
    totals, unused = lax.scan(one_expert, jnp.zeros((TOKENS, D), jnp.float32), jnp.arange(EXPERTS, dtype=jnp.int32))
    return totals.astype(jnp.bfloat16)

def reference(queries, keys, values, head_lambda, out_gain, expert_input, routes, route_weight, moe_gain, gate_weight, up_weight, down_weight):
    mixed_out = attention(queries, keys, values, head_lambda, out_gain)
    expert_mix = experts_part(expert_input, routes, route_weight, moe_gain, gate_weight, up_weight, down_weight)
    return (mixed_out, expert_mix)
```

```python
import functools
import math

import jax
import jax.numpy as jnp
from jax import lax
from jax.experimental import pallas as pl
from jax.experimental.pallas import tpu as pltpu
from jax.sharding import PartitionSpec as P

HEADS = 8
KV_HEADS = 4
HEAD = 64
VDIM = 128


epsilon = 1e-05


def expert_act(rows_in, gate_matrix, up_matrix):
    gate_pre = jnp.dot(rows_in, gate_matrix, preferred_element_type=jnp.float32)
    up_pre = jnp.dot(rows_in, up_matrix, preferred_element_type=jnp.float32)
    clipped = jnp.minimum(gate_pre, 7.0)
    up_clip = jnp.clip(up_pre, -7.0, 7.0)
    return ((up_clip + 1.0) * clipped * jax.nn.sigmoid(1.702 * clipped)).astype(jnp.bfloat16)


def routed_experts(
    expert_input, routes, route_weight, moe_gain, gate_weight, up_weight, down_weight
):
    token_count = expert_input.shape[0]
    top_count = routes.shape[1]
    model_width = expert_input.shape[1]
    ep_count = lax.axis_size("ep")
    capacity = 5 * token_count * top_count // (4 * ep_count)
    inputs_f32 = expert_input.astype(jnp.float32)
    normed = (
        inputs_f32
        * lax.rsqrt(jnp.mean(inputs_f32 * inputs_f32, axis=-1, keepdims=True) + epsilon)
        * moe_gain
    ).astype(jnp.bfloat16)
    flat_routes = routes.reshape(-1)
    route_total = flat_routes.shape[0]
    one_hot = (flat_routes[:, None] == jnp.arange(ep_count, dtype=jnp.int32)[None, :]).astype(
        jnp.int32
    )
    slot_rank = jnp.sum(jnp.cumsum(one_hot, axis=0) * one_hot, axis=1) - 1
    target = flat_routes * capacity + slot_rank
    slot_token = (
        jnp.zeros((ep_count * capacity,), jnp.int32)
        .at[target]
        .set(jnp.arange(route_total, dtype=jnp.int32) // top_count)
    )
    slot_live = jnp.zeros((ep_count * capacity,), jnp.bool_).at[target].set(True)
    outgoing = jnp.where(slot_live[:, None], normed[slot_token], jnp.zeros((), jnp.bfloat16))
    local_gate = gate_weight[0]
    local_up = up_weight[0]
    local_down = down_weight[0]
    arrived = lax.all_to_all(outgoing, "ep", split_axis=0, concat_axis=0, tiled=True)
    activated = expert_act(lax.all_gather(arrived, "tp", axis=0, tiled=True), local_gate, local_up)
    summed = lax.psum_scatter(
        jnp.dot(activated, local_down, preferred_element_type=jnp.float32).astype(jnp.bfloat16),
        "tp",
        scatter_dimension=0,
        tiled=True,
    )
    returned = lax.all_to_all(summed, "ep", split_axis=0, concat_axis=0, tiled=True)
    picked = returned[target].reshape(token_count, top_count, model_width).astype(jnp.float32)
    expert_mix = jnp.sum(route_weight[:, :, None] * picked, axis=1).astype(jnp.bfloat16)
    return expert_mix


def attention_kernel(
    block_len, start_ref, lambda_ref, query_ref, kv_ref, gain_ref, out_ref, spread, sums, peaks
):
    rows = query_ref.shape[0]
    width = 2 * HEAD
    heads = query_ref.shape[1] // width
    kv_heads = kv_ref.shape[1] // (width + VDIM)
    group_size = heads // kv_heads
    lane = lax.broadcasted_iota(jnp.int32, (rows, width), 1)
    for head in range(heads):
        scaled = query_ref[:, head * width : (head + 1) * width] * jnp.bfloat16(HEAD ** (-0.5))
        for which in range(2):
            keep = (lane < HEAD) if which == 0 else (lane >= HEAD)
            spread[2 * head + which] = jnp.where(keep, scaled, jnp.zeros((), jnp.bfloat16))
    sums[...] = jnp.zeros_like(sums)
    peaks[...] = jnp.full_like(peaks, -1e30)
    start = start_ref[0]

    def step(block_index, masked):
        offset = pl.multiple_of(block_index * block_len, block_len)
        for head in range(heads):
            kv_head = head // group_size
            key_block = kv_ref[pl.ds(offset, block_len), kv_head * width : (kv_head + 1) * width]
            base = kv_heads * width + kv_head * VDIM
            value_block = kv_ref[pl.ds(offset, block_len), base : base + VDIM]
            extended = jnp.concatenate(
                [value_block, jnp.ones((block_len, VDIM), jnp.bfloat16)], axis=1
            )
            for which in range(2):
                slot = 2 * head + which
                scores = lax.dot_general(
                    spread[slot],
                    key_block,
                    (((1,), (1,)), ((), ())),
                    preferred_element_type=jnp.float32,
                )
                if masked:
                    query_pos = start + lax.broadcasted_iota(jnp.int32, scores.shape, 0)
                    key_pos = offset + lax.broadcasted_iota(jnp.int32, scores.shape, 1)
                    scores = jnp.where(key_pos <= query_pos, scores, -jnp.inf)
                old_peak = peaks[slot]
                new_peak = jnp.maximum(old_peak, jnp.max(scores, axis=-1, keepdims=True))
                peaks[slot] = new_peak
                factor = jnp.exp(old_peak - new_peak)
                weights = jnp.exp(scores - new_peak[:, :1]).astype(jnp.bfloat16)
                sums[slot] = sums[slot] * jnp.concatenate([factor, factor], axis=1) + jnp.dot(
                    weights, extended, preferred_element_type=jnp.float32
                )

    full = start // block_len

    def full_step(block_index, carry):
        step(block_index, False)
        return carry

    lax.fori_loop(0, full, full_step, 0)

    for extra in range(rows // block_len):
        step(full + extra, True)
    for head in range(heads):
        first, second = sums[2 * head], sums[2 * head + 1]
        combined = (
            first[:, :VDIM] / first[:, VDIM:]
            - lambda_ref[head] * second[:, :VDIM] / second[:, VDIM:]
        )
        inverse_rms = lax.rsqrt(jnp.mean(combined * combined, axis=-1, keepdims=True) + epsilon)
        out_ref[:, head * VDIM : (head + 1) * VDIM] = (
            combined * inverse_rms * gain_ref[...]
        ).astype(jnp.bfloat16)


def attention(queries, keys, values, head_lambda, out_gain):
    rows = queries.shape[0]
    heads = head_lambda.shape[0]
    block_len = math.gcd(rows, 512)
    gathered = lax.all_gather(jnp.concatenate([keys, values], axis=1), "ep", axis=0, tiled=True)
    start = (lax.axis_index("ep") * rows).astype(jnp.int32).reshape(1)
    return pl.pallas_call(
        functools.partial(attention_kernel, block_len),
        out_shape=jax.ShapeDtypeStruct((rows, heads * VDIM), jnp.bfloat16),
        in_specs=[
            pl.BlockSpec(memory_space=pltpu.SMEM),
            pl.BlockSpec(memory_space=pltpu.SMEM),
            pl.BlockSpec(memory_space=pltpu.VMEM),
            pl.BlockSpec(memory_space=pltpu.VMEM),
            pl.BlockSpec(memory_space=pltpu.VMEM),
        ],
        out_specs=pl.BlockSpec(memory_space=pltpu.VMEM),
        scratch_shapes=[
            pltpu.VMEM((2 * heads, rows, 2 * HEAD), jnp.bfloat16),
            pltpu.VMEM((2 * heads, rows, 2 * VDIM), jnp.float32),
            pltpu.VMEM((2 * heads, rows, VDIM), jnp.float32),
        ],
        cost_estimate=pl.CostEstimate(
            flops=16 * rows * gathered.shape[0] * heads * VDIM,
            bytes_accessed=8 * rows * gathered.shape[0],
            transcendentals=2 * rows * gathered.shape[0] * heads,
        ),
    )(start, head_lambda, queries, gathered, out_gain.reshape(1, VDIM))


def dense_experts(
    expert_input, routes, route_weight, moe_gain, gate_weight, up_weight, down_weight
):
    token_count, model_width = expert_input.shape
    ep_count = lax.axis_size("ep")
    chunks = CHUNKS
    inputs_f32 = expert_input.astype(jnp.float32)
    normed = (
        inputs_f32
        * lax.rsqrt(jnp.mean(inputs_f32 * inputs_f32, axis=-1, keepdims=True) + epsilon)
        * moe_gain
    ).astype(jnp.bfloat16)
    table = jnp.sum(
        jnp.where(
            routes[:, :, None] == jnp.arange(ep_count, dtype=jnp.int32)[None, None, :],
            route_weight[:, :, None],
            0.0,
        ),
        axis=1,
    )
    local_gate = gate_weight[0]
    local_up = up_weight[0]
    local_down = down_weight[0]
    both = ("ep", "tp")
    size = token_count // chunks
    arrived = [
        lax.all_gather(normed[at * size : (at + 1) * size], both, axis=0, tiled=True)
        for at in range(chunks)
    ]
    tables = lax.all_gather(table, both, axis=0, tiled=False)
    mine = lax.dynamic_index_in_dim(tables, lax.axis_index("ep"), 2, keepdims=False)
    mixed = []
    for at in range(chunks):
        activated = expert_act(arrived[at], local_gate, local_up)
        weight = mine[:, at * size : (at + 1) * size].reshape(-1, 1)
        product = jnp.dot(activated, local_down, preferred_element_type=jnp.float32)
        mixed.append(
            lax.psum_scatter(
                (product * weight).astype(jnp.bfloat16), both, scatter_dimension=0, tiled=True
            )
        )
    return jnp.concatenate(mixed, axis=0)


CHUNKS = 2


def shards(
    queries,
    keys,
    values,
    head_lambda,
    out_gain,
    expert_input,
    routes,
    route_weight,
    moe_gain,
    gate_weight,
    up_weight,
    down_weight,
):
    mixed_out = attention(queries, keys, values, head_lambda, out_gain)
    dense = lax.axis_size("ep") <= 2 * routes.shape[1]
    experts = dense_experts if dense else routed_experts
    expert_mix = experts(
        expert_input, routes, route_weight, moe_gain, gate_weight, up_weight, down_weight
    )
    return (mixed_out, expert_mix)


def solution(mesh):
    placed = (
        P("ep", "tp"),
        P("ep", "tp"),
        P("ep", "tp"),
        P("tp"),
        P(),
        P(("ep", "tp"), None),
        P(("ep", "tp"), None),
        P(("ep", "tp"), None),
        P(),
        P("ep", None, "tp"),
        P("ep", None, "tp"),
        P("ep", "tp", None),
    )
    return jax.shard_map(
        shards,
        mesh=mesh,
        in_specs=placed,
        out_specs=(P("ep", "tp"), P(("ep", "tp"), None)),
        check_vma=False,
    )
```

```python
import functools
import math

import jax
import jax.numpy as jnp
from jax import lax
from jax.experimental import pallas as pl
from jax.experimental.pallas import tpu as pltpu
from jax.sharding import PartitionSpec as P

HEADS = 8
KV_HEADS = 4
HEAD = 64
VDIM = 128


epsilon = 1e-05


def expert_act(rows_in, gate_matrix, up_matrix):
    gate_pre = jnp.dot(rows_in, gate_matrix, preferred_element_type=jnp.float32)
    up_pre = jnp.dot(rows_in, up_matrix, preferred_element_type=jnp.float32)
    clipped = jnp.minimum(gate_pre, 7.0)
    up_clip = jnp.clip(up_pre, -7.0, 7.0)
    return ((up_clip + 1.0) * clipped * jax.nn.sigmoid(1.702 * clipped)).astype(jnp.bfloat16)


def routed_experts(
    kv_gathered, expert_input, routes, route_weight, moe_gain, gate_weight, up_weight, down_weight
):
    token_count = expert_input.shape[0]
    top_count = routes.shape[1]
    model_width = expert_input.shape[1]
    ep_count = lax.axis_size("ep")
    capacity = 5 * token_count * top_count // (4 * ep_count)
    inputs_f32 = expert_input.astype(jnp.float32)
    normed = (
        inputs_f32
        * lax.rsqrt(jnp.mean(inputs_f32 * inputs_f32, axis=-1, keepdims=True) + epsilon)
        * moe_gain
    ).astype(jnp.bfloat16)
    flat_routes = routes.reshape(-1)
    route_total = flat_routes.shape[0]
    one_hot = (flat_routes[:, None] == jnp.arange(ep_count, dtype=jnp.int32)[None, :]).astype(
        jnp.int32
    )
    slot_rank = jnp.sum(jnp.cumsum(one_hot, axis=0) * one_hot, axis=1) - 1
    target = flat_routes * capacity + slot_rank
    slot_token = (
        jnp.zeros((ep_count * capacity,), jnp.int32)
        .at[target]
        .set(jnp.arange(route_total, dtype=jnp.int32) // top_count)
    )
    slot_live = jnp.zeros((ep_count * capacity,), jnp.bool_).at[target].set(True)
    outgoing = jnp.where(slot_live[:, None], normed[slot_token], jnp.zeros((), jnp.bfloat16))
    local_gate = gate_weight[0]
    local_up = up_weight[0]
    local_down = down_weight[0]
    parts = 2 if capacity % 16 == 0 else 1
    share = capacity // parts
    by_expert = outgoing.reshape(ep_count, capacity, model_width)
    gathered = []
    for part in range(parts):
        sending = by_expert[:, part * share : (part + 1) * share].reshape(-1, model_width)
        arrived = lax.all_to_all(sending, "ep", split_axis=0, concat_axis=0, tiled=True)
        if part == 0:
            arrived, kv_gathered = lax.optimization_barrier((arrived, kv_gathered))
        gathered.append(lax.all_gather(arrived, "tp", axis=0, tiled=True))
    summed = []
    for rows_in in gathered:
        activated = expert_act(rows_in, local_gate, local_up)
        summed.append(
            lax.psum_scatter(
                jnp.dot(activated, local_down, preferred_element_type=jnp.float32).astype(
                    jnp.bfloat16
                ),
                "tp",
                scatter_dimension=0,
                tiled=True,
            )
        )
    returned = jnp.concatenate(
        [
            lax.all_to_all(piece, "ep", split_axis=0, concat_axis=0, tiled=True)
            for piece in summed
        ],
        axis=0,
    )
    part_of = slot_rank // share
    place = part_of * (ep_count * share) + flat_routes * share + slot_rank % share
    by_choice = place.reshape(token_count, top_count).T.reshape(-1)
    picked = returned[by_choice].reshape(top_count, token_count, model_width)
    expert_mix = jnp.sum(
        route_weight.T[:, :, None] * picked.astype(jnp.float32), axis=0
    ).astype(jnp.bfloat16)
    return kv_gathered, expert_mix


def attention_kernel(
    block_len, start_ref, lambda_ref, query_ref, kv_ref, gain_ref, out_ref, spread, sums, peaks
):
    rows = query_ref.shape[0]
    width = 2 * HEAD
    heads = query_ref.shape[1] // width
    kv_heads = kv_ref.shape[1] // (width + VDIM)
    group_size = heads // kv_heads
    lane = lax.broadcasted_iota(jnp.int32, (rows, width), 1)
    for head in range(heads):
        scaled = query_ref[:, head * width : (head + 1) * width] * jnp.bfloat16(HEAD ** (-0.5))
        for which in range(2):
            keep = (lane < HEAD) if which == 0 else (lane >= HEAD)
            spread[2 * head + which] = jnp.where(keep, scaled, jnp.zeros((), jnp.bfloat16))
    sums[...] = jnp.zeros_like(sums)
    peaks[...] = jnp.full_like(peaks, -1e30)
    start = start_ref[0]

    def step(block_index, masked):
        offset = pl.multiple_of(block_index * block_len, block_len)
        for head in range(heads):
            kv_head = head // group_size
            key_block = kv_ref[pl.ds(offset, block_len), kv_head * width : (kv_head + 1) * width]
            base = kv_heads * width + kv_head * VDIM
            value_block = kv_ref[pl.ds(offset, block_len), base : base + VDIM]
            extended = jnp.concatenate(
                [value_block, jnp.ones((block_len, VDIM), jnp.bfloat16)], axis=1
            )
            for which in range(2):
                slot = 2 * head + which
                scores = lax.dot_general(
                    spread[slot],
                    key_block,
                    (((1,), (1,)), ((), ())),
                    preferred_element_type=jnp.float32,
                )
                if masked:
                    query_pos = start + lax.broadcasted_iota(jnp.int32, scores.shape, 0)
                    key_pos = offset + lax.broadcasted_iota(jnp.int32, scores.shape, 1)
                    scores = jnp.where(key_pos <= query_pos, scores, -jnp.inf)
                old_peak = peaks[slot]
                new_peak = jnp.maximum(old_peak, jnp.max(scores, axis=-1, keepdims=True))
                peaks[slot] = new_peak
                factor = jnp.exp(old_peak - new_peak)
                weights = jnp.exp(scores - new_peak[:, :1]).astype(jnp.bfloat16)
                sums[slot] = sums[slot] * jnp.concatenate([factor, factor], axis=1) + jnp.dot(
                    weights, extended, preferred_element_type=jnp.float32
                )

    full = start // block_len

    def full_step(block_index, carry):
        step(block_index, False)
        return carry

    lax.fori_loop(0, full, full_step, 0)

    for extra in range(rows // block_len):
        step(full + extra, True)
    for head in range(heads):
        first, second = sums[2 * head], sums[2 * head + 1]
        combined = (
            first[:, :VDIM] / first[:, VDIM:]
            - lambda_ref[head] * second[:, :VDIM] / second[:, VDIM:]
        )
        inverse_rms = lax.rsqrt(jnp.mean(combined * combined, axis=-1, keepdims=True) + epsilon)
        out_ref[:, head * VDIM : (head + 1) * VDIM] = (
            combined * inverse_rms * gain_ref[...]
        ).astype(jnp.bfloat16)


def attention(queries, gathered, head_lambda, out_gain):
    rows = queries.shape[0]
    heads = head_lambda.shape[0]
    block_len = math.gcd(rows, 512)
    start = (lax.axis_index("ep") * rows).astype(jnp.int32).reshape(1)
    return pl.pallas_call(
        functools.partial(attention_kernel, block_len),
        out_shape=jax.ShapeDtypeStruct((rows, heads * VDIM), jnp.bfloat16),
        in_specs=[
            pl.BlockSpec(memory_space=pltpu.SMEM),
            pl.BlockSpec(memory_space=pltpu.SMEM),
            pl.BlockSpec(memory_space=pltpu.VMEM),
            pl.BlockSpec(memory_space=pltpu.VMEM),
            pl.BlockSpec(memory_space=pltpu.VMEM),
        ],
        out_specs=pl.BlockSpec(memory_space=pltpu.VMEM),
        scratch_shapes=[
            pltpu.VMEM((2 * heads, rows, 2 * HEAD), jnp.bfloat16),
            pltpu.VMEM((2 * heads, rows, 2 * VDIM), jnp.float32),
            pltpu.VMEM((2 * heads, rows, VDIM), jnp.float32),
        ],
        cost_estimate=pl.CostEstimate(
            flops=16 * rows * gathered.shape[0] * heads * VDIM,
            bytes_accessed=8 * rows * gathered.shape[0],
            transcendentals=2 * rows * gathered.shape[0] * heads,
        ),
    )(start, head_lambda, queries, gathered, out_gain.reshape(1, VDIM))


def shards(
    queries,
    keys,
    values,
    head_lambda,
    out_gain,
    expert_input,
    routes,
    route_weight,
    moe_gain,
    gate_weight,
    up_weight,
    down_weight,
):
    kv_gathered = lax.all_gather(
        jnp.concatenate([keys, values], axis=1), "ep", axis=0, tiled=True
    )
    kv_gathered, expert_mix = routed_experts(
        kv_gathered, expert_input, routes, route_weight, moe_gain, gate_weight, up_weight, down_weight
    )
    mixed_out = attention(queries, kv_gathered, head_lambda, out_gain)
    return (mixed_out, expert_mix)


def solution(mesh):
    placed = (
        P("ep", "tp"),
        P("ep", "tp"),
        P("ep", "tp"),
        P("tp"),
        P(),
        P(("ep", "tp"), None),
        P(("ep", "tp"), None),
        P(("ep", "tp"), None),
        P(),
        P("ep", None, "tp"),
        P("ep", None, "tp"),
        P("ep", "tp", None),
    )
    return jax.shard_map(
        shards,
        mesh=mesh,
        in_specs=placed,
        out_specs=(P("ep", "tp"), P(("ep", "tp"), None)),
        check_vma=False,
    )
```
